32 devices in a mesh: ep: 4 (over y, x), tp: 8 (over z, core).
Axes of the slice: x: 2, y: 2, z: 4, core: 2. Of those that a mesh axis runs over, the one named last changes fastest.
Arguments:
- tokens: bfloat16 [128, 4096], P('ep', 'tp'), may hold values from -16 to 16
- routing: int32 [128, 4], P('ep'), may hold values from 0 to 7, all different within a row; in each aligned block of 32 rows (0 to 31, 32 to 63, ...) at most 32 rows name the same one
- gate_weights: float32 [128, 4], P('ep'), may hold values from 0.1 to 1
- w_gate: bfloat16 [8, 1024, 4096], P('ep', 'tp'), may hold values from -0.09375 to 0.09375
- w_up: bfloat16 [8, 1024, 4096], P('ep', 'tp'), may hold values from -0.09375 to 0.09375
- w_down: bfloat16 [8, 1024, 4096], P('ep', None, 'tp'), may hold values from -2 to 2
- out_gain: float32 [4096], P('tp'), may hold values from 0.1 to 1.9
Outputs:
- mixed: bfloat16 [128, 4096], P('ep', 'tp')
The draws below stay inside these ranges and needn't reach their ends.
Inputs may be any that keep to these rules, and one draw needn't show every extreme that they name: `routing`: in each aligned block of 32 rows (the tokens of one index of ep) no expert is named by more than 32 entries, and in every draw some expert is named by exactly 32 entries of some block. The 4 entries of a row differ.
All inputs are finite; a program needn't handle non-finite values.
Results may differ from the reference program's by a relative error of at most 0.0057.
Values may be sent and summed in bfloat16 or wider, within the bound.
No kernel may reach another device: no remote copies, remote signals or barrier semaphores. Data moves between devices by JAX's collectives and lax.ppermute only.
A program may use at most 64 MiB of HBM per device.

```python
import math
import jax
import jax.numpy as jnp
import numpy as np
from jax import lax

D = 4096
FE = 1024
TOPK = 4
EXP_DEV = 2
EXPERTS = 8
TOK_EP = 32
TOKENS = 128
CAP = 32
N_EP = 4


def draw_tokens(key, part):
    first_key, second_key = jax.random.split(key)
    base = jnp.clip(jax.random.normal(first_key, (TOKENS, D), jnp.float32), -4.5, 4.5)
    row_factor = jnp.exp(jax.random.uniform(second_key, (TOKENS, 1), jnp.float32, -1.2, 1.2))
    return (base * row_factor).astype(jnp.bfloat16)


def draw_w_down(key, part):
    first_key, second_key = jax.random.split(jax.random.fold_in(key, 7))
    base = jnp.clip(jax.random.normal(first_key, (EXPERTS, FE, D), jnp.float32), -4.5, 4.5) * FE ** (-0.5)
    group_factor = jnp.exp(jax.random.uniform(second_key, (16,), jnp.float32, -1.1, 1.1))
    column_factor = jnp.repeat(group_factor, D // 16)
    return (base * column_factor[None, None, :]).astype(jnp.bfloat16)


def block_levels(rng, shape, shards, low, largest):
    loudness = 1.0
    for position, parts in shards:
        heights = jax.random.uniform(jax.random.fold_in(jax.random.fold_in(rng, 6), position), (parts,), jnp.float32, low / len(shards), largest / len(shards))
        loudness = loudness * jnp.repeat(jnp.exp(heights), shape[position] // parts).reshape((-1,) + (1,) * (len(shape) - 1 - position))
    return loudness


def deal_out(own_key, own, number, rows, number_of, top, bound, lean):
    order = jax.random.permutation(own_key, number_of)
    packed, usual = portions_of(number_of, rows * top, bound, lean, True), portions_of(number_of, rows * top, bound, lean, False)
    places = jnp.arange(number_of)

    def named(tallies, offset_by):
        used = int((tallies > 0).sum())
        fixed = max(1, used // 4)
        moved = fixed + (places - fixed + offset_by * (used - fixed)) % max(1, number_of - fixed)
        return jnp.zeros((number_of,), jnp.int32).at[order[jnp.where(places < fixed, places, moved)]].set(jnp.asarray(tallies, jnp.int32))

    tallies = jnp.where(number % 4 == 0, named(packed, number // 4), named(usual, number - number // 4 - 1))
    mixed = jax.random.permutation(jax.random.fold_in(own, 3), number_of)
    giver, receiver = mixed[0:number_of // 2 * 2:2], mixed[1:number_of // 2 * 2:2]
    slack = jnp.minimum(tallies[giver] - 1, bound - tallies[receiver]) // 2
    slack = jnp.where((giver == order[0]) | (receiver == order[0]) | (tallies[receiver] == 0), 0, jnp.maximum(slack, 0))
    moved = jax.random.randint(jax.random.fold_in(own, 4), (number_of // 2,), 0, 1 << 20) % (slack + 1)
    tallies = tallies.at[giver].add(-moved).at[receiver].add(moved)
    labels = jnp.searchsorted(jnp.cumsum(tallies), jnp.arange(rows * top), side="right").astype(jnp.int32)
    grid = labels.reshape(top, rows).T
    grid = grid[jax.random.permutation(jax.random.fold_in(own, 1), rows)]
    offset_by = jax.random.randint(jax.random.fold_in(own, 2), (rows, 1), 0, top)
    return jnp.take_along_axis(grid, (jnp.arange(top)[None, :] + offset_by) % top, axis=1)


def portions_of(number_of, total, bound, skew, full):
    portions = [(1 << 20) // math.isqrt(grade ** skew) + 1 for grade in range(1, number_of + 1)]
    largest = bound if full else min(bound, max(-(-total // number_of), total * portions[0] // sum(portions)))
    least = 1 if total - largest >= number_of - 1 else 0
    given, spare = [largest] + [least] * (number_of - 1), total - largest - least * (number_of - 1)
    while spare > 0:
        candidates = [i for i in range(1, number_of) if given[i] < largest] or [i for i in range(1, number_of) if given[i] < bound]
        whole, budget = sum([portions[i] for i in candidates]), spare
        for i in candidates:
            extra = min(bound - given[i], max(1, budget * portions[i] // whole), spare)
            given[i] = given[i] + extra
            spare = spare - extra
    return np.array(given)


def scatter_about(own_key, extent, scale, reach, cuts=(), kind=jnp.bfloat16):
    factor_of = block_levels(own_key, extent, cuts, -0.22, 0.18) if cuts else 1.0
    drawn = jax.random.normal(own_key, extent, jnp.float32) * scale * factor_of
    return jnp.minimum(jnp.maximum(drawn, -reach), reach).astype(kind)


def setup_inputs(seed: int = 0) -> dict:
    key_of = jax.random.split(jax.random.key(seed), 8)
    tokens = draw_tokens(jax.random.fold_in(key_of[7], 71), 0)
    routing_keys = jax.random.split(jax.random.fold_in(key_of[1], 1), TOKENS // TOK_EP)
    routing_turns = jax.random.permutation(jax.random.fold_in(key_of[1], 3), TOKENS // TOK_EP)
    routing = jax.vmap(lambda own, number: deal_out(jax.random.fold_in(key_of[1], 2), own, number, TOK_EP, EXPERTS, TOPK, CAP, 2))(routing_keys, routing_turns).reshape((TOKENS, TOPK))
    gate_weights = jnp.clip(0.1 + 0.9 * jax.random.uniform(key_of[2], (TOKENS, TOPK), jnp.float32) ** block_levels(key_of[2], (TOKENS, TOPK), ((0, 4),), -0.2, 0.2), 0.1, 1.0)
    w_gate = scatter_about(key_of[3], (EXPERTS, FE, D), D ** -0.5, 0.09375, ((0, 4), (1, 8)))
    w_up = scatter_about(key_of[4], (EXPERTS, FE, D), D ** -0.5, 0.09375, ((0, 4), (1, 8)))
    w_down = draw_w_down(jax.random.fold_in(key_of[7], 71), 0)
    out_gain = jnp.clip(1.0 + 0.18 * jax.random.normal(key_of[6], (D,), jnp.float32), 0.1, 1.9)
    return {"tokens": tokens, "routing": routing, "gate_weights": gate_weights, "w_gate": w_gate, "w_up": w_up, "w_down": w_down, "out_gain": out_gain}


norm_eps = 1e-05

def reference(tokens, routing, gate_weights, w_gate, w_up, w_down, out_gain):
    experts = EXP_DEV * N_EP
    rows_max = N_EP * CAP
    token_f = tokens.astype(jnp.float32)
    row_scale = lax.rsqrt(lax.optimization_barrier(jnp.mean(token_f * token_f, axis=1)) + norm_eps)
    flat_route = routing.reshape(-1).astype(jnp.int32)
    entry_count = flat_route.shape[0]
    expert_ids = jnp.arange(experts, dtype=jnp.int32)
    hit_table = (flat_route[:, None] == expert_ids[None, :]).astype(jnp.int32)
    running = jnp.cumsum(hit_table, axis=0).astype(jnp.int32) - hit_table
    slot_rank = lax.optimization_barrier(jnp.sum(running * hit_table, axis=1)).astype(jnp.int32)
    owner = (jnp.arange(entry_count, dtype=jnp.int32) // TOPK).astype(jnp.int32)

    def one_expert(inputs):
        expert_id, gate_mat, up_mat, down_mat = inputs
        target = jnp.where(flat_route == expert_id, slot_rank, rows_max).astype(jnp.int32)
        row_ids = jnp.zeros((rows_max,), jnp.int32).at[target].set(owner, mode='drop')
        picked_rows = tokens[row_ids]
        scale_rows = row_scale[row_ids][:, None]
        gate_pre = jnp.dot(picked_rows, gate_mat.T, preferred_element_type=jnp.float32) * scale_rows
        up_pre = jnp.dot(picked_rows, up_mat.T, preferred_element_type=jnp.float32) * scale_rows
        hidden = (jax.nn.silu(gate_pre) * up_pre).astype(jnp.bfloat16)
        return jnp.dot(hidden, down_mat, preferred_element_type=jnp.float32).astype(jnp.bfloat16)
    expert_outs = lax.map(one_expert, (expert_ids, w_gate, w_up, w_down))
    chosen = expert_outs[flat_route, slot_rank].astype(jnp.float32).reshape(TOKENS, TOPK, D)
    combined = lax.optimization_barrier(jnp.sum(chosen * gate_weights[:, :, None], axis=1))
    final_scale = lax.rsqrt(lax.optimization_barrier(jnp.mean(combined * combined, axis=1)) + norm_eps)
    return (combined * final_scale[:, None] * out_gain[None, :]).astype(jnp.bfloat16)
```

```python
import jax
import jax.numpy as jnp
from jax import lax
from jax.experimental import pallas as pl
from jax.experimental.pallas import tpu as pltpu
from jax.sharding import PartitionSpec as P

D = 4096
TOPK = 4
EXP_DEV = 2


norm_eps = 1e-05


def routed_body(tokens, routing, gate_weights, w_gate, w_up, w_down, out_gain):
    ep_count = lax.axis_size("ep")
    tok_rows = tokens.shape[0]
    width_part = tokens.shape[1]
    experts = EXP_DEV * ep_count
    slot_count = 2 * tok_rows * TOPK // experts
    span_rows = ep_count * slot_count
    total_slots = EXP_DEV * span_rows
    flat_route = routing.reshape(-1)
    expert_ids = jnp.arange(experts, dtype=jnp.int32)
    hit_table = (flat_route[:, None] == expert_ids[None, :]).astype(jnp.int32)
    running = jnp.cumsum(hit_table, axis=0) - hit_table
    slot_rank = jnp.sum(running * hit_table, axis=1)
    slot_target = flat_route % EXP_DEV * span_rows + flat_route // EXP_DEV * slot_count + slot_rank
    entry_targets = slot_target.reshape(tok_rows, TOPK)
    slot_ids = jnp.arange(total_slots, dtype=jnp.int32)
    select_table = jnp.any(entry_targets[None, :, :] == slot_ids[:, None, None], axis=2).astype(
        jnp.bfloat16
    )
    outgoing = jnp.dot(select_table, tokens, preferred_element_type=jnp.float32).astype(
        jnp.bfloat16
    )
    outgoing = outgoing.reshape(EXP_DEV, ep_count, slot_count, width_part)
    arrived = lax.all_to_all(outgoing, "ep", split_axis=1, concat_axis=1, tiled=True).reshape(
        EXP_DEV, span_rows, width_part
    )
    piece_cols = lax.all_gather(arrived, "tp", axis=2, tiled=True)
    gate_sum = jnp.einsum("efn,esn->efs", w_gate, piece_cols, preferred_element_type=jnp.float32)
    up_sum = jnp.einsum("efn,esn->efs", w_up, piece_cols, preferred_element_type=jnp.float32)
    square_sum = jnp.einsum(
        "esn,esn->es", piece_cols, piece_cols, preferred_element_type=jnp.float32
    )
    row_scale = lax.rsqrt(square_sum / D + norm_eps)[:, None, :]
    hidden = (jax.nn.silu(gate_sum * row_scale) * (up_sum * row_scale)).astype(jnp.bfloat16)
    out_part = w_down.shape[2]
    expert_out = jnp.einsum(
        "ens,end->esd",
        lax.all_gather(hidden, "tp", axis=1, tiled=True),
        w_down,
        preferred_element_type=jnp.float32,
    ).astype(jnp.bfloat16)
    returned = lax.all_to_all(
        expert_out.reshape(EXP_DEV, ep_count, slot_count, out_part),
        "ep",
        split_axis=1,
        concat_axis=1,
        tiled=True,
    )
    returned = returned.reshape(total_slots, out_part)
    chosen = returned[slot_target].astype(jnp.float32).reshape(tok_rows, TOPK, out_part)
    combined = jnp.sum(chosen * gate_weights[:, :, None], axis=1)
    square_total = lax.psum(jnp.sum(combined * combined, axis=1), "tp")
    final_scale = lax.rsqrt(square_total / D + norm_eps)
    return (combined * final_scale[:, None] * out_gain[None, :]).astype(jnp.bfloat16)


def swap_pairs(count, mask):
    return [(i, i ^ mask) for i in range(count)]


def gather_swapped(x, axis, masks):
    count = lax.axis_size(axis)
    return [x] + [lax.ppermute(x, axis, swap_pairs(count, mask)) for mask in masks]


def hidden_kernel(place_ref, own_ref, pair_ref, coef_ref, gate_ref, up_ref, out_ref):
    eps, chips, rows, part = own_ref.shape
    experts, units, width = gate_ref.shape
    gate_sum = jnp.zeros((eps * rows, experts * units), jnp.float32)
    up_sum = jnp.zeros((eps * rows, experts * units), jnp.float32)
    square_sum = jnp.zeros((eps * rows, 128), jnp.float32)
    contract = (((1,), (1,)), ((), ()))
    for from_pair, ref in enumerate((own_ref, pair_ref)):
        for step in range(chips):
            piece = ref[:, step].reshape(eps * rows, part)
            block = ((place_ref[0] // 2) ^ step) * 2 + ((place_ref[0] % 2) ^ from_pair)
            cols = pl.ds(pl.multiple_of(block * part, part), part)
            gate_part = gate_ref[:, :, cols].reshape(experts * units, part)
            up_part = up_ref[:, :, cols].reshape(experts * units, part)
            gate_sum += lax.dot_general(piece, gate_part, contract, preferred_element_type=jnp.float32)
            up_sum += lax.dot_general(piece, up_part, contract, preferred_element_type=jnp.float32)
            wide = piece.astype(jnp.float32)
            wide = wide * wide
            for first in range(0, part, 128):
                square_sum += wide[:, first : first + 128]
    row_scale = lax.rsqrt(jnp.sum(square_sum, axis=1, keepdims=True) / width + norm_eps)
    coef = coef_ref[...].reshape(eps * rows, experts)
    for e in range(experts):
        cols = slice(e * units, (e + 1) * units)
        gate_pre = gate_sum[:, cols] * row_scale
        up_pre = up_sum[:, cols] * row_scale
        silu = gate_pre / (1.0 + jnp.exp(-gate_pre))
        out_ref[:, cols] = (silu * up_pre * coef[:, e : e + 1]).astype(out_ref.dtype)


def down_kernel(place_ref, own_ref, pair_ref, down_ref, out_ref):
    chips, rows, _ = own_ref.shape
    experts, _, part = down_ref.shape
    units = own_ref.shape[2] // experts
    total = jnp.zeros((rows, part), jnp.float32)
    for from_pair, ref in enumerate((own_ref, pair_ref)):
        for step in range(chips):
            block = ((place_ref[0] // 2) ^ step) * 2 + ((place_ref[0] % 2) ^ from_pair)
            span = pl.ds(pl.multiple_of(block * units, units), units)
            for e in range(experts):
                total += jnp.dot(
                    ref[step, :, e * units : (e + 1) * units],
                    down_ref[e, span, :],
                    preferred_element_type=jnp.float32,
                )
    out_ref[...] = total.reshape(out_ref.shape).astype(out_ref.dtype)


def call_local(kernel, out, *operands):
    vmem = pl.BlockSpec(memory_space=pltpu.VMEM)
    smem = pl.BlockSpec(memory_space=pltpu.SMEM)
    return pl.pallas_call(
        kernel,
        out_shape=out,
        in_specs=[smem] + [vmem] * (len(operands) - 1),
        out_specs=vmem,
    )(*operands)


def dense_body(tokens, routing, gate_weights, w_gate, w_up, w_down, out_gain):
    eps = lax.axis_size("ep")
    parts = lax.axis_size("tp")
    rows, width_part = tokens.shape
    experts, units, width = w_gate.shape
    chip_masks = range(2, parts, 2)
    ep_masks = range(1, eps)
    ep_index = lax.axis_index("ep")
    place = lax.axis_index("tp").astype(jnp.int32).reshape(1)

    def coef_for(mask):
        ids = (ep_index ^ mask) * experts + jnp.arange(experts, dtype=jnp.int32)
        hits = routing[:, :, None] == ids[None, None, :]
        return jnp.sum(jnp.where(hits, gate_weights[:, :, None], 0.0), axis=1)

    coef = jnp.stack(
        [coef_for(0)]
        + [lax.ppermute(coef_for(m), "ep", swap_pairs(eps, m)) for m in ep_masks]
    )
    own = jnp.stack(gather_swapped(tokens, "tp", chip_masks))
    own = jnp.stack(gather_swapped(own, "ep", ep_masks))
    pair = lax.ppermute(own, "tp", swap_pairs(parts, 1))
    hidden = call_local(
        hidden_kernel,
        jax.ShapeDtypeStruct((eps * rows, experts * units), jnp.bfloat16),
        place, own, pair, coef, w_gate, w_up,
    )
    own = jnp.stack(gather_swapped(hidden, "tp", chip_masks))
    pair = lax.ppermute(own, "tp", swap_pairs(parts, 1))
    partial = call_local(
        down_kernel,
        jax.ShapeDtypeStruct((eps, rows, w_down.shape[2]), jnp.bfloat16),
        place, own, pair, w_down,
    )
    combined = partial[0].astype(jnp.float32)
    for m in ep_masks:
        combined += lax.ppermute(partial[m], "ep", swap_pairs(eps, m)).astype(jnp.float32)
    square_sum = jnp.sum(combined * combined, axis=1)
    square_sum += lax.ppermute(square_sum, "tp", swap_pairs(parts, 1))
    square_sum = sum(gather_swapped(square_sum, "tp", chip_masks))
    final_scale = lax.rsqrt(square_sum / width + norm_eps)
    return (combined * final_scale[:, None] * out_gain[None, :]).astype(jnp.bfloat16)


def body(tokens, routing, *rest):
    eps = lax.axis_size("ep")
    parts = lax.axis_size("tp")
    rows = tokens.shape[0]
    experts = EXP_DEV * eps
    slot_count = 2 * rows * TOPK // experts
    powers = all(n & (n - 1) == 0 for n in (eps, parts))
    if slot_count >= rows and powers and parts > 1:
        return dense_body(tokens, routing, *rest)
    return routed_body(tokens, routing, *rest)


def solution(mesh):
    placed = (
        P("ep", "tp"),
        P("ep", None),
        P("ep", None),
        P("ep", "tp", None),
        P("ep", "tp", None),
        P("ep", None, "tp"),
        P("tp"),
    )
    return jax.shard_map(body, mesh=mesh, in_specs=placed, out_specs=P("ep", "tp"), check_vma=False)
```

```python
import jax
import jax.numpy as jnp
from jax import lax
from jax.experimental import pallas as pl
from jax.experimental.pallas import tpu as pltpu
from jax.sharding import PartitionSpec as P

D = 4096
TOPK = 4
EXP_DEV = 2


norm_eps = 1e-05


def routed_body(tokens, routing, gate_weights, w_gate, w_up, w_down, out_gain):
    ep_count = lax.axis_size("ep")
    tok_rows = tokens.shape[0]
    width_part = tokens.shape[1]
    experts = EXP_DEV * ep_count
    slot_count = 2 * tok_rows * TOPK // experts
    span_rows = ep_count * slot_count
    total_slots = EXP_DEV * span_rows
    flat_route = routing.reshape(-1)
    expert_ids = jnp.arange(experts, dtype=jnp.int32)
    hit_table = (flat_route[:, None] == expert_ids[None, :]).astype(jnp.int32)
    running = jnp.cumsum(hit_table, axis=0) - hit_table
    slot_rank = jnp.sum(running * hit_table, axis=1)
    slot_target = flat_route % EXP_DEV * span_rows + flat_route // EXP_DEV * slot_count + slot_rank
    entry_targets = slot_target.reshape(tok_rows, TOPK)
    slot_ids = jnp.arange(total_slots, dtype=jnp.int32)
    select_table = jnp.any(entry_targets[None, :, :] == slot_ids[:, None, None], axis=2).astype(
        jnp.bfloat16
    )
    outgoing = jnp.dot(select_table, tokens, preferred_element_type=jnp.float32).astype(
        jnp.bfloat16
    )
    outgoing = outgoing.reshape(EXP_DEV, ep_count, slot_count, width_part)
    arrived = lax.all_to_all(outgoing, "ep", split_axis=1, concat_axis=1, tiled=True).reshape(
        EXP_DEV, span_rows, width_part
    )
    piece_cols = lax.all_gather(arrived, "tp", axis=2, tiled=True)
    gate_sum = jnp.einsum("efn,esn->efs", w_gate, piece_cols, preferred_element_type=jnp.float32)
    up_sum = jnp.einsum("efn,esn->efs", w_up, piece_cols, preferred_element_type=jnp.float32)
    square_sum = jnp.einsum(
        "esn,esn->es", piece_cols, piece_cols, preferred_element_type=jnp.float32
    )
    row_scale = lax.rsqrt(square_sum / D + norm_eps)[:, None, :]
    hidden = (jax.nn.silu(gate_sum * row_scale) * (up_sum * row_scale)).astype(jnp.bfloat16)
    out_part = w_down.shape[2]
    expert_out = jnp.einsum(
        "ens,end->esd",
        lax.all_gather(hidden, "tp", axis=1, tiled=True),
        w_down,
        preferred_element_type=jnp.float32,
    ).astype(jnp.bfloat16)
    returned = lax.all_to_all(
        expert_out.reshape(EXP_DEV, ep_count, slot_count, out_part),
        "ep",
        split_axis=1,
        concat_axis=1,
        tiled=True,
    )
    returned = returned.reshape(total_slots, out_part)
    chosen = returned[slot_target].astype(jnp.float32).reshape(tok_rows, TOPK, out_part)
    combined = jnp.sum(chosen * gate_weights[:, :, None], axis=1)
    square_total = lax.psum(jnp.sum(combined * combined, axis=1), "tp")
    final_scale = lax.rsqrt(square_total / D + norm_eps)
    return (combined * final_scale[:, None] * out_gain[None, :]).astype(jnp.bfloat16)


def swap_pairs(count, mask):
    return [(i, i ^ mask) for i in range(count)]


def gather_swapped(x, axis, masks):
    count = lax.axis_size(axis)
    return [x] + [lax.ppermute(x, axis, swap_pairs(count, mask)) for mask in masks]


def stack_kernel(count):
    def kernel(*refs):
        for i in range(count):
            refs[-1][i] = refs[i][...]

    return kernel


def stack_local(pieces, *after):
    vmem = pl.BlockSpec(memory_space=pltpu.VMEM)
    return pl.pallas_call(
        stack_kernel(len(pieces)),
        out_shape=jax.ShapeDtypeStruct((len(pieces),) + pieces[0].shape, pieces[0].dtype),
        in_specs=[vmem] * (len(pieces) + len(after)),
        out_specs=vmem,
        compiler_params=pltpu.CompilerParams(vmem_limit_bytes=8 << 20),
    )(*pieces, *after)


def touch_kernel(place_ref, gate_ref, up_ref, out_ref):
    out_ref[...] = gate_ref[0, :16, :128] + up_ref[0, :16, :128]


def coef_kernel(place_ref, routing_ref, weights_ref, *out_refs):
    routing = routing_ref[...]
    weights = weights_ref[...]
    for mask, out_ref in enumerate(out_refs):
        experts = out_ref.shape[1]
        first = (place_ref[0] ^ mask) * experts
        for e in range(experts):
            hit = jnp.where(routing == first + e, weights, 0.0)
            out_ref[:, e : e + 1] = jnp.sum(hit, axis=1, keepdims=True)


def sum_pieces(place_ref, from_pair, ref, gate_ref, up_ref, gate_sum, up_sum, square_sum):
    eps, chips, rows, part = ref.shape
    experts, units, _ = gate_ref.shape
    contract = (((1,), (1,)), ((), ()))
    for step in range(chips):
        piece = ref[:, step].reshape(eps * rows, part)
        block = ((place_ref[0] // 2) ^ step) * 2 + ((place_ref[0] % 2) ^ from_pair)
        cols = pl.ds(pl.multiple_of(block * part, part), part)
        gate_part = gate_ref[:, :, cols].reshape(experts * units, part)
        up_part = up_ref[:, :, cols].reshape(experts * units, part)
        gate_sum += lax.dot_general(piece, gate_part, contract, preferred_element_type=jnp.float32)
        up_sum += lax.dot_general(piece, up_part, contract, preferred_element_type=jnp.float32)
        wide = piece.astype(jnp.float32)
        wide = wide * wide
        for first in range(0, part, 128):
            square_sum += wide[:, first : first + 128]
    return gate_sum, up_sum, square_sum


def own_half_kernel(place_ref, own_ref, gate_ref, up_ref, gate_out, up_out, square_out):
    zeros = [jnp.zeros(ref.shape, jnp.float32) for ref in (gate_out, up_out, square_out)]
    gate_out[...], up_out[...], square_out[...] = sum_pieces(
        place_ref, 0, own_ref, gate_ref, up_ref, *zeros
    )


def hidden_kernel(place_ref, pair_ref, gate_ref, up_ref, gate_in, up_in, square_in, *rest):
    *coef_refs, out_ref = rest
    experts, units, width = gate_ref.shape
    gate_sum, up_sum, square_sum = sum_pieces(
        place_ref, 1, pair_ref, gate_ref, up_ref, gate_in[...], up_in[...], square_in[...]
    )
    row_scale = lax.rsqrt(jnp.sum(square_sum, axis=1, keepdims=True) / width + norm_eps)
    coef = jnp.concatenate([ref[...] for ref in coef_refs], axis=0)
    for e in range(experts):
        cols = slice(e * units, (e + 1) * units)
        gate_pre = gate_sum[:, cols] * row_scale
        up_pre = up_sum[:, cols] * row_scale
        silu = gate_pre / (1.0 + jnp.exp(-gate_pre))
        out_ref[:, cols] = (silu * up_pre * coef[:, e : e + 1]).astype(out_ref.dtype)


def down_kernel(place_ref, own_ref, pair_ref, down_ref, *out_refs):
    chips, rows, _ = own_ref.shape
    experts, _, part = down_ref.shape
    units = own_ref.shape[2] // experts
    total = jnp.zeros((rows, part), jnp.float32)
    for from_pair, ref in enumerate((own_ref, pair_ref)):
        for step in range(chips):
            block = ((place_ref[0] // 2) ^ step) * 2 + ((place_ref[0] % 2) ^ from_pair)
            span = pl.ds(pl.multiple_of(block * units, units), units)
            for e in range(experts):
                total += jnp.dot(
                    ref[step, :, e * units : (e + 1) * units],
                    down_ref[e, span, :],
                    preferred_element_type=jnp.float32,
                )
    for i, out_ref in enumerate(out_refs):
        tokens = out_ref.shape[0]
        out_ref[...] = total[i * tokens : (i + 1) * tokens].astype(out_ref.dtype)


def call_local(kernel, limit, outs, *operands):
    vmem = pl.BlockSpec(memory_space=pltpu.VMEM)
    smem = pl.BlockSpec(memory_space=pltpu.SMEM)
    return pl.pallas_call(
        kernel,
        out_shape=outs,
        in_specs=[smem] + [vmem] * (len(operands) - 1),
        out_specs=[vmem] * len(outs),
        compiler_params=pltpu.CompilerParams(vmem_limit_bytes=limit),
    )(*operands)


def dense_body(tokens, routing, gate_weights, w_gate, w_up, w_down, out_gain):
    eps = lax.axis_size("ep")
    parts = lax.axis_size("tp")
    rows, width_part = tokens.shape
    experts, units, width = w_gate.shape
    part = w_down.shape[2]
    chip_masks = range(2, parts, 2)
    ep_masks = range(1, eps)
    ep_place = lax.axis_index("ep").astype(jnp.int32).reshape(1)
    place = lax.axis_index("tp").astype(jnp.int32).reshape(1)
    pieces = gather_swapped(tokens, "tp", chip_masks)
    coefs = call_local(
        coef_kernel,
        8 << 20,
        [jax.ShapeDtypeStruct((rows, experts), jnp.float32)] * eps,
        ep_place, routing, gate_weights,
    )
    coefs = list(coefs[:1]) + [
        lax.ppermute(coefs[m], "ep", swap_pairs(eps, m)) for m in ep_masks
    ]
    touched = call_local(
        touch_kernel, 16 << 20, [jax.ShapeDtypeStruct((16, 128), w_gate.dtype)],
        place, w_gate, w_up,
    )
    own = stack_local(pieces, *coefs, *touched)
    own = stack_local(gather_swapped(own, "ep", ep_masks))
    pair = lax.ppermute(own, "tp", swap_pairs(parts, 1))
    sums = jax.ShapeDtypeStruct((eps * rows, experts * units), jnp.float32)
    squares = jax.ShapeDtypeStruct((eps * rows, 128), jnp.float32)
    sums = call_local(
        own_half_kernel, 16 << 20, [sums, sums, squares], place, own, w_gate, w_up
    )
    (hidden,) = call_local(
        hidden_kernel,
        16 << 20,
        [jax.ShapeDtypeStruct((eps * rows, experts * units), jnp.bfloat16)],
        place, pair, w_gate, w_up, *sums, *coefs,
    )
    own = stack_local(gather_swapped(hidden, "tp", chip_masks))
    pair = lax.ppermute(own, "tp", swap_pairs(parts, 1))
    combined, *others = call_local(
        down_kernel,
        8 << 20,
        [jax.ShapeDtypeStruct((rows, part), jnp.float32)]
        + [jax.ShapeDtypeStruct((rows, part), jnp.bfloat16)] * (eps - 1),
        place, own, pair, w_down,
    )
    for m, other in zip(ep_masks, others):
        combined += lax.ppermute(other, "ep", swap_pairs(eps, m)).astype(jnp.float32)
    square_sum = jnp.sum(combined * combined, axis=1)
    square_sum += lax.ppermute(square_sum, "tp", swap_pairs(parts, 1))
    square_sum = sum(gather_swapped(square_sum, "tp", chip_masks))
    final_scale = lax.rsqrt(square_sum / width + norm_eps)
    return (combined * final_scale[:, None] * out_gain[None, :]).astype(jnp.bfloat16)


def body(tokens, routing, *rest):
    eps = lax.axis_size("ep")
    parts = lax.axis_size("tp")
    rows = tokens.shape[0]
    experts = EXP_DEV * eps
    slot_count = 2 * rows * TOPK // experts
    powers = all(n & (n - 1) == 0 for n in (eps, parts))
    if slot_count >= rows and powers and parts > 1:
        return dense_body(tokens, routing, *rest)
    return routed_body(tokens, routing, *rest)


def solution(mesh):
    placed = (
        P("ep", "tp"),
        P("ep", None),
        P("ep", None),
        P("ep", "tp", None),
        P("ep", "tp", None),
        P("ep", None, "tp"),
        P("tp"),
    )
    return jax.shard_map(body, mesh=mesh, in_specs=placed, out_specs=P("ep", "tp"), check_vma=False)
```

```python
import jax
import jax.numpy as jnp
from jax import lax
from jax.experimental import pallas as pl
from jax.experimental.pallas import tpu as pltpu
from jax.sharding import PartitionSpec as P

D = 4096
TOPK = 4
EXP_DEV = 2


norm_eps = 1e-05


def routed_body(tokens, routing, gate_weights, w_gate, w_up, w_down, out_gain):
    ep_count = lax.axis_size("ep")
    tok_rows = tokens.shape[0]
    width_part = tokens.shape[1]
    experts = EXP_DEV * ep_count
    slot_count = 2 * tok_rows * TOPK // experts
    span_rows = ep_count * slot_count
    total_slots = EXP_DEV * span_rows
    flat_route = routing.reshape(-1)
    expert_ids = jnp.arange(experts, dtype=jnp.int32)
    hit_table = (flat_route[:, None] == expert_ids[None, :]).astype(jnp.int32)
    running = jnp.cumsum(hit_table, axis=0) - hit_table
    slot_rank = jnp.sum(running * hit_table, axis=1)
    slot_target = flat_route % EXP_DEV * span_rows + flat_route // EXP_DEV * slot_count + slot_rank
    entry_targets = slot_target.reshape(tok_rows, TOPK)
    slot_ids = jnp.arange(total_slots, dtype=jnp.int32)
    select_table = jnp.any(entry_targets[None, :, :] == slot_ids[:, None, None], axis=2).astype(
        jnp.bfloat16
    )
    outgoing = jnp.dot(select_table, tokens, preferred_element_type=jnp.float32).astype(
        jnp.bfloat16
    )
    outgoing = outgoing.reshape(EXP_DEV, ep_count, slot_count, width_part)
    arrived = lax.all_to_all(outgoing, "ep", split_axis=1, concat_axis=1, tiled=True).reshape(
        EXP_DEV, span_rows, width_part
    )
    piece_cols = lax.all_gather(arrived, "tp", axis=2, tiled=True)
    gate_sum = jnp.einsum("efn,esn->efs", w_gate, piece_cols, preferred_element_type=jnp.float32)
    up_sum = jnp.einsum("efn,esn->efs", w_up, piece_cols, preferred_element_type=jnp.float32)
    square_sum = jnp.einsum(
        "esn,esn->es", piece_cols, piece_cols, preferred_element_type=jnp.float32
    )
    row_scale = lax.rsqrt(square_sum / D + norm_eps)[:, None, :]
    hidden = (jax.nn.silu(gate_sum * row_scale) * (up_sum * row_scale)).astype(jnp.bfloat16)
    out_part = w_down.shape[2]
    expert_out = jnp.einsum(
        "ens,end->esd",
        lax.all_gather(hidden, "tp", axis=1, tiled=True),
        w_down,
        preferred_element_type=jnp.float32,
    ).astype(jnp.bfloat16)
    returned = lax.all_to_all(
        expert_out.reshape(EXP_DEV, ep_count, slot_count, out_part),
        "ep",
        split_axis=1,
        concat_axis=1,
        tiled=True,
    )
    returned = returned.reshape(total_slots, out_part)
    chosen = returned[slot_target].astype(jnp.float32).reshape(tok_rows, TOPK, out_part)
    combined = jnp.sum(chosen * gate_weights[:, :, None], axis=1)
    square_total = lax.psum(jnp.sum(combined * combined, axis=1), "tp")
    final_scale = lax.rsqrt(square_total / D + norm_eps)
    return (combined * final_scale[:, None] * out_gain[None, :]).astype(jnp.bfloat16)


def swap_pairs(count, mask):
    return [(i, i ^ mask) for i in range(count)]


def gather_swapped(x, axis, masks):
    count = lax.axis_size(axis)
    far_first = sorted(masks, key=lambda mask: -min(mask, count - mask))
    got = {mask: lax.ppermute(x, axis, swap_pairs(count, mask)) for mask in far_first}
    return [x] + [got[mask] for mask in masks]


def gather_relayed(x, axis, masks):
    if len(masks) != 3:
        return gather_swapped(x, axis, masks)
    count = lax.axis_size(axis)
    near = lax.ppermute(x, axis, swap_pairs(count, masks[0]))
    back = lax.ppermute(x, axis, swap_pairs(count, masks[2]))
    far = lax.ppermute(near, axis, swap_pairs(count, masks[2]))
    return [x, near, far, back]


def stack_kernel(count):
    def kernel(*refs):
        for i in range(count):
            refs[-1][i] = refs[i][...]

    return kernel


def stack_local(pieces, *after):
    vmem = pl.BlockSpec(memory_space=pltpu.VMEM)
    return pl.pallas_call(
        stack_kernel(len(pieces)),
        out_shape=jax.ShapeDtypeStruct((len(pieces),) + pieces[0].shape, pieces[0].dtype),
        in_specs=[vmem] * (len(pieces) + len(after)),
        out_specs=vmem,
        compiler_params=pltpu.CompilerParams(vmem_limit_bytes=8 << 20),
    )(*pieces, *after)


def touch_kernel(place_ref, gate_ref, up_ref, after_ref, out_ref):
    out_ref[...] = gate_ref[0, :16, :128] + up_ref[0, :16, :128]


def coef_kernel(place_ref, routing_ref, weights_ref, *out_refs):
    routing = routing_ref[...]
    weights = weights_ref[...]
    for mask, out_ref in enumerate(out_refs):
        experts = out_ref.shape[1]
        first = (place_ref[0] ^ mask) * experts
        for e in range(experts):
            hit = jnp.where(routing == first + e, weights, 0.0)
            out_ref[:, e : e + 1] = jnp.sum(hit, axis=1, keepdims=True)


def sum_pieces(place_ref, from_pair, ref, gate_ref, up_ref, gate_sum, up_sum, square_sum):
    eps, chips, rows, part = ref.shape
    experts, units, _ = gate_ref.shape
    contract = (((1,), (1,)), ((), ()))
    for step in range(chips):
        piece = ref[:, step].reshape(eps * rows, part)
        block = ((place_ref[0] // 2) ^ step) * 2 + ((place_ref[0] % 2) ^ from_pair)
        cols = pl.ds(pl.multiple_of(block * part, part), part)
        gate_part = gate_ref[:, :, cols].reshape(experts * units, part)
        up_part = up_ref[:, :, cols].reshape(experts * units, part)
        gate_sum += lax.dot_general(piece, gate_part, contract, preferred_element_type=jnp.float32)
        up_sum += lax.dot_general(piece, up_part, contract, preferred_element_type=jnp.float32)
        wide = piece.astype(jnp.float32)
        wide = wide * wide
        for first in range(0, part, 128):
            square_sum += wide[:, first : first + 128]
    return gate_sum, up_sum, square_sum


def own_half_kernel(place_ref, own_ref, gate_ref, up_ref, gate_out, up_out, square_out):
    zeros = [jnp.zeros(ref.shape, jnp.float32) for ref in (gate_out, up_out, square_out)]
    gate_out[...], up_out[...], square_out[...] = sum_pieces(
        place_ref, 0, own_ref, gate_ref, up_ref, *zeros
    )


def hidden_kernel(place_ref, pair_ref, gate_ref, up_ref, gate_in, up_in, square_in, *rest):
    *coef_refs, out_ref = rest
    experts, units, width = gate_ref.shape
    gate_sum, up_sum, square_sum = sum_pieces(
        place_ref, 1, pair_ref, gate_ref, up_ref, gate_in[...], up_in[...], square_in[...]
    )
    row_scale = lax.rsqrt(jnp.sum(square_sum, axis=1, keepdims=True) / width + norm_eps)
    coef = jnp.concatenate([ref[...] for ref in coef_refs], axis=0)
    for e in range(experts):
        cols = slice(e * units, (e + 1) * units)
        gate_pre = gate_sum[:, cols] * row_scale
        up_pre = up_sum[:, cols] * row_scale
        silu = gate_pre / (1.0 + jnp.exp(-gate_pre))
        out_ref[:, cols] = (silu * up_pre * coef[:, e : e + 1]).astype(out_ref.dtype)


def down_kernel(place_ref, own_ref, pair_ref, down_ref, *out_refs):
    chips, rows, _ = own_ref.shape
    experts, _, part = down_ref.shape
    units = own_ref.shape[2] // experts
    total = jnp.zeros((rows, part), jnp.float32)
    for from_pair, ref in enumerate((own_ref, pair_ref)):
        for step in range(chips):
            block = ((place_ref[0] // 2) ^ step) * 2 + ((place_ref[0] % 2) ^ from_pair)
            span = pl.ds(pl.multiple_of(block * units, units), units)
            for e in range(experts):
                total += jnp.dot(
                    ref[step, :, e * units : (e + 1) * units],
                    down_ref[e, span, :],
                    preferred_element_type=jnp.float32,
                )
    for i, out_ref in enumerate(out_refs):
        tokens = out_ref.shape[0]
        out_ref[...] = total[i * tokens : (i + 1) * tokens].astype(out_ref.dtype)


def call_local(kernel, limit, outs, *operands):
    vmem = pl.BlockSpec(memory_space=pltpu.VMEM)
    smem = pl.BlockSpec(memory_space=pltpu.SMEM)
    return pl.pallas_call(
        kernel,
        out_shape=outs,
        in_specs=[smem] + [vmem] * (len(operands) - 1),
        out_specs=[vmem] * len(outs),
        compiler_params=pltpu.CompilerParams(vmem_limit_bytes=limit),
    )(*operands)


def dense_body(tokens, routing, gate_weights, w_gate, w_up, w_down, out_gain):
    eps = lax.axis_size("ep")
    parts = lax.axis_size("tp")
    rows, width_part = tokens.shape
    experts, units, width = w_gate.shape
    part = w_down.shape[2]
    chip_masks = range(2, parts, 2)
    ep_masks = range(1, eps)
    ep_place = lax.axis_index("ep").astype(jnp.int32).reshape(1)
    place = lax.axis_index("tp").astype(jnp.int32).reshape(1)
    pieces = gather_swapped(tokens, "tp", chip_masks)
    coefs = call_local(
        coef_kernel,
        8 << 20,
        [jax.ShapeDtypeStruct((rows, experts), jnp.float32)] * eps,
        ep_place, routing, gate_weights,
    )
    coefs = list(coefs[:1]) + [
        lax.ppermute(coefs[m], "ep", swap_pairs(eps, m)) for m in ep_masks
    ]
    own = stack_local(pieces, *coefs)
    touched = call_local(
        touch_kernel, 16 << 20, [jax.ShapeDtypeStruct((16, 128), w_gate.dtype)],
        place, w_gate, w_up, own,
    )
    own = stack_local(gather_swapped(own, "ep", ep_masks), *touched)
    pair = lax.ppermute(own, "tp", swap_pairs(parts, 1))
    sums = jax.ShapeDtypeStruct((eps * rows, experts * units), jnp.float32)
    squares = jax.ShapeDtypeStruct((eps * rows, 128), jnp.float32)
    sums = call_local(
        own_half_kernel, 16 << 20, [sums, sums, squares], place, own, w_gate, w_up
    )
    (hidden,) = call_local(
        hidden_kernel,
        16 << 20,
        [jax.ShapeDtypeStruct((eps * rows, experts * units), jnp.bfloat16)],
        place, pair, w_gate, w_up, *sums, *coefs,
    )
    own = stack_local(gather_relayed(hidden, "tp", chip_masks))
    pair = lax.ppermute(own, "tp", swap_pairs(parts, 1))
    combined, *others = call_local(
        down_kernel,
        8 << 20,
        [jax.ShapeDtypeStruct((rows, part), jnp.float32)]
        + [jax.ShapeDtypeStruct((rows, part), jnp.bfloat16)] * (eps - 1),
        place, own, pair, w_down,
    )
    for m, other in zip(ep_masks, others):
        combined += lax.ppermute(other, "ep", swap_pairs(eps, m)).astype(jnp.float32)
    square_sum = jnp.sum(combined * combined, axis=1)
    square_sum += lax.ppermute(square_sum, "tp", swap_pairs(parts, 1))
    square_sum = sum(gather_swapped(square_sum, "tp", chip_masks))
    final_scale = lax.rsqrt(square_sum / width + norm_eps)
    return (combined * final_scale[:, None] * out_gain[None, :]).astype(jnp.bfloat16)


def body(tokens, routing, *rest):
    eps = lax.axis_size("ep")
    parts = lax.axis_size("tp")
    rows = tokens.shape[0]
    experts = EXP_DEV * eps
    slot_count = 2 * rows * TOPK // experts
    powers = all(n & (n - 1) == 0 for n in (eps, parts))
    if slot_count >= rows and powers and parts > 1:
        return dense_body(tokens, routing, *rest)
    return routed_body(tokens, routing, *rest)


def solution(mesh):
    placed = (
        P("ep", "tp"),
        P("ep", None),
        P("ep", None),
        P("ep", "tp", None),
        P("ep", "tp", None),
        P("ep", None, "tp"),
        P("tp"),
    )
    return jax.shard_map(body, mesh=mesh, in_specs=placed, out_specs=P("ep", "tp"), check_vma=False)
```
